32 devices in a mesh: ra: 4 (over z), cb: 2 (over y), dp: 4 (over x, core).
Axes of the slice: x: 2, y: 2, z: 4, core: 2. Of those that a mesh axis runs over, the one named last changes fastest.
Arguments:
- stream: bfloat16 [1024, 2048], P('dp', 'ra'), may hold values from -60 to 60
- norm_gain: float32 [2, 2048], P(None, 'ra'), may hold values from 0.1 to 1.9
- gate_weight: float32 [2, 2048, 5504], P(None, 'ra', 'cb'), may hold values from -0.125 to 0.125
- up_weight: float32 [2, 2048, 5504], P(None, 'ra', 'cb'), may hold values from -0.125 to 0.125
- down_weight: float32 [2, 5504, 2048], P(None, 'cb', 'ra'), may hold values from -0.078125 to 0.078125
- gate_scale: float32 [2, 5504], P(None, 'cb'), may hold values from 0.5 to 2
- up_scale: float32 [2, 5504], P(None, 'cb'), may hold values from 0.5 to 2
- down_scale: float32 [2, 2048], P(None, 'ra'), may hold values from 0.5 to 2
Outputs:
- result: bfloat16 [1024, 2048], P('dp', 'ra')
The draws below stay inside these ranges and needn't reach their ends.
All inputs are finite; a program needn't handle non-finite values.
Results may differ from the reference program's by a relative error of at most 0.04.
Values may be sent and summed in bfloat16 or wider, within the bound.
No kernel may reach another device: no remote copies, remote signals or barrier semaphores. Data moves between devices by JAX's collectives and lax.ppermute only.
A program may use at most 128 MiB of HBM per device.

```python
import math
import jax
import jax.numpy as jnp
from jax import lax

D = 2048
FF = 5504
TOKENS = 1024
N_RA = 4


def draw_stream(key, part):
    keys = jax.random.split(jax.random.fold_in(key, 11), 3)
    position = jnp.arange(D).astype(jnp.float32) / D
    column_scale = 0.3 * 10.0 ** position * jax.random.uniform(keys[0], (D,), jnp.float32, 0.7, 1.4)
    row_scale = 10.0 ** jax.random.uniform(keys[1], (TOKENS, 1), jnp.float32, -0.5, 0.5)
    base = jnp.clip(jax.random.normal(keys[2], (TOKENS, D), jnp.float32), -4.0, 4.0)
    return (base * row_scale * column_scale).astype(jnp.bfloat16)


def level_of(key, dims, cuts, low, largest):
    level = 1.0
    for dim, blocks in cuts:
        heights = jax.random.uniform(jax.random.fold_in(jax.random.fold_in(key, 6), dim), (blocks,), jnp.float32, low / len(cuts), largest / len(cuts))
        level = level * jnp.repeat(jnp.exp(heights), dims[dim] // blocks).reshape((-1,) + (1,) * (len(dims) - 1 - dim))
    return level


def centred(rng, shape, scale, reach, shards=(), dtype=jnp.bfloat16):
    loudness = level_of(rng, shape, shards, -0.22, 0.18) if shards else 1.0
    drawn = jax.random.normal(rng, shape, jnp.float32) * scale * loudness
    return jnp.minimum(jnp.maximum(drawn, -reach), reach).astype(dtype)


def setup_inputs(seed: int = 0) -> dict:
    splits = jax.random.split(jax.random.key(seed), 9)
    stream = draw_stream(jax.random.fold_in(splits[8], 71), 0)
    norm_gain = jnp.clip(1.0 + 0.18 * jax.random.normal(splits[1], (2, D), jnp.float32), 0.1, 1.9)
    gate_weight = centred(splits[2], (2, D, FF), D ** -0.5, 0.125, ((1, 4), (2, 2)), jnp.float32)
    up_weight = centred(splits[3], (2, D, FF), D ** -0.5, 0.125, ((1, 4), (2, 2)), jnp.float32)
    down_weight = centred(splits[4], (2, FF, D), FF ** -0.5, 0.078125, ((1, 2), (2, 4)), jnp.float32)
    gate_scale = jnp.clip(jnp.exp(math.log(2.0) - 1.3862944 * jax.random.uniform(splits[5], (2, FF), jnp.float32) ** level_of(splits[5], (2, FF), ((1, 2),), -0.2, 0.2)), 0.5, 2.0)
    up_scale = jnp.clip(jnp.exp(math.log(2.0) - 1.3862944 * jax.random.uniform(splits[6], (2, FF), jnp.float32) ** level_of(splits[6], (2, FF), ((1, 2),), -0.2, 0.2)), 0.5, 2.0)
    down_scale = jnp.clip(jnp.exp(math.log(2.0) - 1.3862944 * jax.random.uniform(splits[7], (2, D), jnp.float32) ** level_of(splits[7], (2, D), ((1, 4),), -0.2, 0.2)), 0.5, 2.0)
    return {"stream": stream, "norm_gain": norm_gain, "gate_weight": gate_weight, "up_weight": up_weight, "down_weight": down_weight, "gate_scale": gate_scale, "up_scale": up_scale, "down_scale": down_scale}


epsilon = 1e-06
residual_scale = 0.5

def block_sums(normed, weight):
    width = D // N_RA

    def add_block(carry, index):
        start = (index * width).astype(jnp.int32)
        columns = lax.dynamic_slice_in_dim(normed, start, width, 1)
        rows = lax.dynamic_slice_in_dim(weight, start, width, 0)
        piece = jnp.dot(columns, rows, preferred_element_type=jnp.float32).astype(jnp.bfloat16)
        piece = lax.optimization_barrier(piece)
        return (carry + piece.astype(jnp.float32), None)
    initial = jnp.zeros((normed.shape[0], weight.shape[1]), jnp.float32)
    total, unused = lax.scan(add_block, initial, jnp.arange(N_RA).astype(jnp.int32))
    return total

def half_step(stream, gain, gate_weight, up_weight, down_weight, gate_scale, up_scale, down_scale):
    widened = stream.astype(jnp.float32)
    squares = lax.optimization_barrier(jnp.sum(widened * widened, axis=1, keepdims=True))
    inverse = lax.rsqrt(squares / D + epsilon)
    normed = (widened * gain).astype(jnp.bfloat16)
    gate_sum = block_sums(normed, gate_weight.astype(jnp.bfloat16)) * inverse * gate_scale
    up_sum = block_sums(normed, up_weight.astype(jnp.bfloat16)) * inverse * up_scale
    hidden = (jax.nn.silu(gate_sum) * up_sum).astype(jnp.bfloat16)
    branch = jnp.dot(hidden, down_weight.astype(jnp.bfloat16), preferred_element_type=jnp.float32) * down_scale
    return (residual_scale * widened + branch).astype(jnp.bfloat16)

def reference(stream, norm_gain, gate_weight, up_weight, down_weight, gate_scale, up_scale, down_scale):
    current = stream
    for block_index in range(2):
        current = half_step(current, norm_gain[block_index], gate_weight[block_index], up_weight[block_index], down_weight[block_index], gate_scale[block_index], up_scale[block_index], down_scale[block_index])
    return current
```

```python
import jax
import jax.numpy as jnp
from jax import lax
from jax.sharding import PartitionSpec as P


epsilon = 1e-06
residual_scale = 0.5
GROUPS = 1
f32 = jnp.float32
bf16 = jnp.bfloat16


def sum_small(value, axis, n):
    total = value
    for shift in range(1, n):
        total = total + lax.ppermute(value, axis, [(i, (i + shift) % n) for i in range(n)])
    return total


def sum_columns(partial, n):
    if n == 1:
        return partial
    if n != 2:
        return lax.psum(partial, "cb")
    own = lax.reduce_precision(partial, 8, 7)
    other = lax.ppermute(own.astype(bf16), "cb", [(0, 1), (1, 0)])
    return own + other.astype(f32)


def half_step(group, width, n, n_cb, gain, weights, gate_scale, up_scale, down_scale):
    gate_weight, up_weight, down_weight = weights
    widened = group.astype(f32)
    normed = (widened * gain).astype(bf16)
    gate = jnp.dot(normed, gate_weight, preferred_element_type=f32).astype(bf16)
    up = jnp.dot(normed, up_weight, preferred_element_type=f32).astype(bf16)
    squares = sum_small(jnp.sum(widened * widened, axis=1), "ra", n)
    rows = group.shape[0] // n
    gate_part = lax.psum_scatter(gate, "ra", scatter_dimension=0, tiled=True).astype(f32)
    up_part = lax.psum_scatter(up, "ra", scatter_dimension=0, tiled=True).astype(f32)
    own_squares = lax.dynamic_slice_in_dim(squares, lax.axis_index("ra") * rows, rows, 0)
    inverse = lax.rsqrt(own_squares / width + epsilon)[:, None]
    gate_sum = gate_part * inverse * gate_scale
    up_sum = up_part * inverse * up_scale
    own_hidden = (jax.nn.silu(gate_sum) * up_sum).astype(bf16)
    hidden = lax.all_gather(own_hidden, "ra", axis=0, tiled=True)
    partial = jnp.dot(hidden, down_weight, preferred_element_type=f32)
    branch = sum_columns(partial, n_cb) * down_scale
    return (residual_scale * widened + branch).astype(bf16)


def solution(mesh):
    n, n_cb = mesh.shape["ra"], mesh.shape["cb"]

    def on_device(
        stream, norm_gain, gate_weight, up_weight, down_weight, gate_scale, up_scale, down_scale
    ):
        width = stream.shape[1] * n
        groups = jnp.split(stream, GROUPS, 0)
        for b in range(2):
            weights = (gate_weight[b], up_weight[b], down_weight[b])
            weights = tuple(w.astype(bf16) for w in weights)
            groups = [
                half_step(
                    group, width, n, n_cb, norm_gain[b], weights,
                    gate_scale[b], up_scale[b], down_scale[b],
                )
                for group in groups
            ]
        return jnp.concatenate(groups, 0)

    in_specs = (
        P("dp", "ra"),
        P(None, "ra"),
        P(None, "ra", "cb"),
        P(None, "ra", "cb"),
        P(None, "cb", "ra"),
        P(None, "cb"),
        P(None, "cb"),
        P(None, "ra"),
    )
    return jax.shard_map(
        on_device, mesh=mesh, in_specs=in_specs, out_specs=P("dp", "ra"), check_vma=False
    )
```
